256 devices in a mesh: sp: 16 (over y, x), tp: 16 (over z, core).
Axes of the slice: x: 4, y: 4, z: 8, core: 2. Of those that a mesh axis runs over, the one named last changes fastest.
Arguments:
- queries: bfloat16 [6144, 2048], P('sp', 'tp'), may hold values from -6 to 6
- keys: bfloat16 [6144, 2048], P('sp', 'tp'), may hold values from -6 to 6
- values: bfloat16 [6144, 2048], P('sp', 'tp'), may hold values from -6 to 6
- key_bias: bfloat16 [6144, 32], P('sp', 'tp'), may hold values from -16 to 0
- head_gain: float32 [32, 64], P('tp'), may hold values from 0.1 to 1.9
- out_weight: bfloat16 [2048, 2048], P('tp'), may hold values from -0.125 to 0.125
- residual: bfloat16 [6144, 2048], P(('sp', 'tp')), may hold values from -6 to 6
- norm_gain: float32 [2048], replicated, may hold values from 0.1 to 1.9
- gate_proj: bfloat16 [16, 2048, 7168], P('sp', None, 'tp'), may hold values from -0.125 to 0.125
- up_proj: bfloat16 [16, 2048, 7168], P('sp', None, 'tp'), may hold values from -0.125 to 0.125
- down_proj: bfloat16 [16, 7168, 2048], P('sp', 'tp'), may hold values from -0.0625 to 0.0625
- expert_choice: int32 [6144, 2], P(('sp', 'tp')), may hold values from 0 to 15, all different within a row; in each aligned block of 24 rows (0 to 23, 24 to 47, ...) at most 6 rows name the same one
- expert_weights: float32 [6144, 2], P(('sp', 'tp')), may hold values from 0.2 to 1
Outputs:
- layer_out: bfloat16 [6144, 2048], P(('sp', 'tp'))
The draws below stay inside these ranges and needn't reach their ends.
Inputs may be any that keep to these rules, and one draw needn't show every extreme that they name: `expert_choice`: in each aligned block of 24 rows (the rows of one device), no expert is named more than 6 times; the two experts of a row differ.
All inputs are finite; a program needn't handle non-finite values.
Results may differ from the reference program's by a relative error of at most 0.019.
Values may be sent and summed in bfloat16 or wider, within the bound.
No kernel may reach another device: no remote copies, remote signals or barrier semaphores. Data moves between devices by JAX's collectives and lax.ppermute only.
A program may use at most 128 MiB of HBM per device.

```python
import math
import jax
import jax.numpy as jnp
import numpy as np
from jax import lax

D = 2048
HEADS = 32
HEAD_DIM = 64
FFE = 7168
TOK_DEV = 384
TOKENS = 6144
EXPERTS = 16
ROWS_DEV = 24
CAP = 6
N_TP = 16


def draw_key_bias(key, part):
    streams = jax.random.split(jax.random.fold_in(key, 11), 7)
    chance = 0.5
    slow_heads = jax.random.uniform(streams[0], (HEADS,)) < chance
    fast_base = jax.random.uniform(streams[1], (HEADS,), minval=-5.0, maxval=-3.8)
    slow_base = -jnp.log(jnp.float32(TOKENS)) - 0.5 + jax.random.uniform(streams[2], (HEADS,), minval=-0.5, maxval=0.5)
    blocks = TOKENS // TOK_DEV
    device_factor = jax.random.uniform(streams[3], (blocks, 1, HEADS), minval=-0.7, maxval=0.7)
    device_factor = jnp.broadcast_to(device_factor, (blocks, TOK_DEV, HEADS)).reshape(TOKENS, HEADS)
    jitter = 0.3 * jax.random.normal(streams[4], (TOKENS, HEADS))
    base = jnp.where(slow_heads[None, :], slow_base[None, :], fast_base[None, :]) + device_factor + jitter
    spots = jax.random.randint(streams[5], (2,), 0, TOKENS)
    levels = jax.random.uniform(streams[6], (2, HEADS), minval=-1.4, maxval=0.0)
    position = jnp.arange(TOKENS)
    first_hit = (position == spots[0])[:, None] & slow_heads[None, :]
    second_hit = (position == spots[1])[:, None] & slow_heads[None, :]
    base = jnp.where(first_hit, levels[0][None, :], base)
    base = jnp.where(second_hit, levels[1][None, :], base)
    return jnp.clip(base, -16.0, 0.0).astype(jnp.bfloat16)


def block_levels(stream_key, extent, pieces, smallest, top_value):
    factor_of, own = 1.0, jax.random.fold_in(stream_key, 6)
    for dim, blocks in pieces:
        heights = jnp.exp(jax.random.uniform(jax.random.fold_in(own, dim), (blocks,), jnp.float32, smallest / len(pieces), top_value / len(pieces)))
        factor_of = factor_of * jnp.repeat(heights, extent[dim] // blocks).reshape([-1 if axis == dim else 1 for axis in range(len(extent))])
    return factor_of


def assign_block(key, own, number, rows, count, top, bound, skew):
    sequence = jax.random.permutation(key, count)
    heavy_load, ordinary = shares(count, rows * top, bound, skew, True), shares(count, rows * top, bound, skew, False)
    places = jnp.arange(count)

    def named(tallies, rotation):
        used = int((tallies > 0).sum())
        fixed = max(1, used // 4)
        shifted = fixed + (places - fixed + rotation * (used - fixed)) % max(1, count - fixed)
        return jnp.zeros((count,), jnp.int32).at[sequence[jnp.where(places < fixed, places, shifted)]].set(jnp.asarray(tallies, jnp.int32))

    tallies = jnp.where(number % 4 == 0, named(heavy_load, number // 4), named(ordinary, number - number // 4 - 1))
    mixed = jax.random.permutation(jax.random.fold_in(own, 3), count)
    giver, taker = mixed[0:count // 2 * 2:2], mixed[1:count // 2 * 2:2]
    margin = jnp.minimum(tallies[giver] - 1, bound - tallies[taker]) // 2
    margin = jnp.where((giver == sequence[0]) | (taker == sequence[0]) | (tallies[taker] == 0), 0, jnp.maximum(margin, 0))
    shifted = jax.random.randint(jax.random.fold_in(own, 4), (count // 2,), 0, 1 << 20) % (margin + 1)
    tallies = tallies.at[giver].add(-shifted).at[taker].add(shifted)
    items = jnp.searchsorted(jnp.cumsum(tallies), jnp.arange(rows * top), side="right").astype(jnp.int32)
    table = items.reshape(top, rows).T
    table = table[jax.random.permutation(jax.random.fold_in(own, 1), rows)]
    rotation = jax.random.randint(jax.random.fold_in(own, 2), (rows, 1), 0, top)
    return jnp.take_along_axis(table, (jnp.arange(top)[None, :] + rotation) % top, axis=1)


def shares(count, total, limit, slope, full):
    weights = [(1 << 20) // math.isqrt(standing ** slope) + 1 for standing in range(1, count + 1)]
    largest = limit if full else min(limit, max(-(-total // count), total * weights[0] // sum(weights)))
    least = 1 if total - largest >= count - 1 else 0
    counts, spare = [largest] + [least] * (count - 1), total - largest - least * (count - 1)
    while spare > 0:
        movable = [i for i in range(1, count) if counts[i] < largest] or [i for i in range(1, count) if counts[i] < limit]
        whole, remaining = sum([weights[i] for i in movable]), spare
        for i in movable:
            addition = min(limit - counts[i], max(1, remaining * weights[i] // whole), spare)
            counts[i] = counts[i] + addition
            spare = spare - addition
    return np.array(counts)


def scatter_about(key, shape, spread, reach, shards=(), held_as=jnp.bfloat16):
    gain = block_levels(key, shape, shards, -0.22, 0.18) if shards else 1.0
    values = jax.random.normal(key, shape, jnp.float32) * spread * gain
    return jnp.minimum(jnp.maximum(values, -reach), reach).astype(held_as)


def setup_inputs(seed: int = 0) -> dict:
    key_of = jax.random.split(jax.random.key(seed), 14)
    queries = scatter_about(key_of[0], (TOKENS, HEADS * HEAD_DIM), 1.0, 6.0, ((0, 16), (1, 16)))
    keys = scatter_about(key_of[1], (TOKENS, HEADS * HEAD_DIM), 1.0, 6.0, ((0, 16), (1, 16)))
    values = scatter_about(key_of[2], (TOKENS, HEADS * HEAD_DIM), 1.0, 6.0, ((0, 16), (1, 16)))
    key_bias = draw_key_bias(jax.random.fold_in(key_of[13], 71), 0)
    head_gain = jnp.clip(1.0 + 0.18 * jax.random.normal(key_of[4], (HEADS, HEAD_DIM), jnp.float32), 0.1, 1.9)
    out_weight = scatter_about(key_of[5], (HEADS * HEAD_DIM, D), (HEADS * HEAD_DIM) ** -0.5, 0.125, ((0, 16),))
    residual = scatter_about(key_of[6], (TOKENS, D), 1.0, 6.0, ((0, 256),))
    norm_gain = jnp.clip(1.0 + 0.18 * jax.random.normal(key_of[7], (D,), jnp.float32), 0.1, 1.9)
    gate_proj = scatter_about(key_of[8], (EXPERTS, D, FFE), D ** -0.5, 0.125, ((0, 16), (2, 16)))
    up_proj = scatter_about(key_of[9], (EXPERTS, D, FFE), D ** -0.5, 0.125, ((0, 16), (2, 16)))
    down_proj = scatter_about(key_of[10], (EXPERTS, FFE, D), FFE ** -0.5, 0.0625, ((0, 16), (1, 16)))
    expert_choice_keys = jax.random.split(jax.random.fold_in(key_of[11], 1), TOKENS // ROWS_DEV)
    expert_choice_turns = jax.random.permutation(jax.random.fold_in(key_of[11], 3), TOKENS // ROWS_DEV)
    expert_choice = jax.vmap(lambda own, number: assign_block(jax.random.fold_in(key_of[11], 2), own, number, ROWS_DEV, EXPERTS, 2, CAP, 1))(expert_choice_keys, expert_choice_turns).reshape((TOKENS, 2))
    expert_weights = jnp.clip(0.2 + 0.8 * jax.random.uniform(key_of[12], (TOKENS, 2), jnp.float32) ** block_levels(key_of[12], (TOKENS, 2), ((0, 256),), -0.2, 0.2), 0.2, 1.0)
    return {"queries": queries, "keys": keys, "values": values, "key_bias": key_bias, "head_gain": head_gain, "out_weight": out_weight, "residual": residual, "norm_gain": norm_gain, "gate_proj": gate_proj, "up_proj": up_proj, "down_proj": down_proj, "expert_choice": expert_choice, "expert_weights": expert_weights}


epsilon = 1e-06

def rms_scaled(values_in):
    return values_in * lax.rsqrt(lax.optimization_barrier(jnp.mean(values_in * values_in, axis=-1, keepdims=True)) + epsilon)

def head_mixture(operands):
    query_head, key_head, value_head, bias_head = operands
    length = query_head.shape[0]
    blocks = length // TOK_DEV
    scores = jnp.dot(query_head, key_head.T, preferred_element_type=jnp.float32) * HEAD_DIM ** (-0.5)
    scores = scores + bias_head.astype(jnp.float32)[None, :]
    position = jnp.arange(length, dtype=jnp.int32)
    earlier = (position[None, :] < position[:, None]).reshape(length, blocks, TOK_DEV)
    scores = scores.reshape(length, blocks, TOK_DEV)
    log_drops = jnp.where(earlier, jax.nn.log_sigmoid(-scores), 0.0)
    suffix = lax.cumsum(log_drops, axis=2, reverse=True) - log_drops
    within = jnp.where(earlier, jnp.exp(jax.nn.log_sigmoid(scores) + suffix), 0.0).astype(jnp.bfloat16)
    value_blocks = value_head.reshape(blocks, TOK_DEV, HEAD_DIM).astype(jnp.float32)
    block_sums = jnp.einsum('tms,msd->tmd', within.astype(jnp.float32), value_blocks)
    totals = lax.optimization_barrier(jnp.sum(log_drops, axis=2))
    carried = lax.optimization_barrier(jnp.sum(totals, axis=1, keepdims=True)) - jnp.cumsum(totals, axis=1)
    return lax.optimization_barrier(jnp.sum(jnp.exp(carried)[:, :, None] * block_sums, axis=1))

def reference(queries, keys, values, key_bias, head_gain, out_weight, residual, norm_gain, gate_proj, up_proj, down_proj, expert_choice, expert_weights):

    def split_heads(array):
        return array.reshape(TOKENS, HEADS, HEAD_DIM).transpose(1, 0, 2)
    mixture = lax.map(head_mixture, (split_heads(queries), split_heads(keys), split_heads(values), key_bias.T))
    attended = (rms_scaled(mixture) * head_gain[:, None, :]).astype(jnp.bfloat16)
    attended = attended.transpose(1, 0, 2).reshape(TOKENS, HEADS * HEAD_DIM)
    projected = jnp.dot(attended, out_weight, preferred_element_type=jnp.float32)
    stream = (residual.astype(jnp.float32) + projected).astype(jnp.bfloat16)
    normed = (rms_scaled(stream.astype(jnp.float32)) * norm_gain).astype(jnp.bfloat16)
    device_blocks = TOKENS // ROWS_DEV
    flat_expert = expert_choice.reshape(-1).astype(jnp.int32)
    flat_token = jnp.arange(2 * TOKENS, dtype=jnp.int32) // 2
    onehot = (flat_expert[:, None] == jnp.arange(EXPERTS, dtype=jnp.int32)[None, :]).astype(jnp.int32)
    grouped = onehot.reshape(device_blocks, 2 * ROWS_DEV, EXPERTS)
    before = (jnp.cumsum(grouped, axis=1) - grouped).reshape(2 * TOKENS, EXPERTS)
    slot_rank = lax.optimization_barrier(jnp.sum(before * onehot, axis=1)).astype(jnp.int32)
    slot_index = (flat_token // ROWS_DEV * CAP + slot_rank).astype(jnp.int32)
    slot_table = jnp.full((EXPERTS, device_blocks * CAP), TOKENS, jnp.int32).at[flat_expert, slot_index].set(flat_token)
    padded = jnp.concatenate([normed, jnp.zeros((1, D), jnp.bfloat16)], axis=0)
    group_size = FFE // N_TP

    def one_expert(operands):
        rows_index, gate_matrix, up_matrix, down_matrix = operands
        row_block = padded[rows_index]
        gate_part = jnp.dot(row_block, gate_matrix, preferred_element_type=jnp.float32)
        up_part = jnp.dot(row_block, up_matrix, preferred_element_type=jnp.float32)
        hidden = (jax.nn.silu(gate_part) * up_part).astype(jnp.bfloat16)
        hidden_groups = hidden.reshape(row_block.shape[0], N_TP, group_size).transpose(1, 0, 2)
        down_groups = down_matrix.reshape(N_TP, group_size, D)

        def add_group(running, group_pair):
            rounded = jnp.dot(group_pair[0], group_pair[1], preferred_element_type=jnp.float32).astype(jnp.bfloat16)
            rounded = lax.optimization_barrier(rounded)
            return (running + rounded.astype(jnp.float32), None)
        running, unused = lax.scan(add_group, jnp.zeros((row_block.shape[0], D), jnp.float32), (hidden_groups, down_groups))
        return running.astype(jnp.bfloat16)
    expert_out = lax.map(one_expert, (slot_table, gate_proj, up_proj, down_proj))
    picked = expert_out[flat_expert, slot_index].astype(jnp.float32).reshape(TOKENS, 2, D)
    combined = lax.optimization_barrier(jnp.sum(expert_weights[:, :, None] * picked, axis=1))
    return (stream.astype(jnp.float32) + combined).astype(jnp.bfloat16)
```

```python
import jax
import jax.numpy as jnp
from jax import lax
from jax.experimental import pallas as pl
from jax.experimental.pallas import tpu as pltpu
from jax.sharding import PartitionSpec as P

epsilon = 1e-06
BLOCK = 384
HEAD = 64
PIECE = BLOCK + 16
RING = 8

PARTNER = [(i, 15 - i) for i in range(16)]
Y_SWAP = [(i, i ^ 4) for i in range(16)]
X_NEXT = [(i, i // 4 * 4 + (i + 1) % 4) for i in range(16)]
X_BACK = [(i, i // 4 * 4 + (i + 3) % 4) for i in range(16)]
Z_NEXT = [(i, (i + 2) % 16) for i in range(16)]
Z_BACK = [(i, (i + 14) % 16) for i in range(16)]
CORE_SWAP = [(i, i ^ 1) for i in range(16)]
SAME_CORE = [[2 * z + c for z in range(RING)] for c in range(2)]


def rms_scaled(values_in):
    return values_in * lax.rsqrt(jnp.mean(values_in * values_in, axis=-1, keepdims=True) + epsilon)


def choice_ranks(routes, experts_all):
    flat_routes = routes.reshape(routes.shape[:-2] + (-1,))
    onehot = (flat_routes[..., None] == jnp.arange(experts_all, dtype=jnp.int32)).astype(jnp.int32)
    before = jnp.cumsum(onehot, axis=-2) - onehot
    return jnp.sum(before * onehot, axis=-1).reshape(routes.shape)


def slot_tokens(slot_index, targets, missing):
    flat_slots = slot_index.reshape(-1)
    owners = jnp.arange(flat_slots.shape[0], dtype=jnp.int32) // 2
    matches = flat_slots[None, :] == jnp.arange(targets, dtype=jnp.int32)[:, None]
    owner_found = jnp.sum(jnp.where(matches, owners[None, :], 0), axis=1)
    return jnp.where(jnp.any(matches, axis=1), owner_found, missing)


def attention_kernel(rank_ref, q_own, q_other, *rest):
    pieces, (gain_ref, out_ref, kv, bias, later, acc, total) = rest[:8], rest[8:]
    rank = rank_ref[0]
    for j in range(8):
        for half in range(2):
            start = half * PIECE
            kv[2 * j + half] = pieces[j][start : start + BLOCK, :]
            bias[2 * j + half] = pieces[j][start + BLOCK : start + PIECE, :].astype(jnp.float32)
    row = lax.broadcasted_iota(jnp.int32, (BLOCK, BLOCK + 128), 0)
    col = lax.broadcasted_iota(jnp.int32, (BLOCK, BLOCK + 128), 1)
    later[...] = jnp.where((row >= col) | (col >= BLOCK), 1.0, 0.0).astype(jnp.bfloat16)

    def slot_of(block):
        mirrored = (block // 8) != (rank // 8)
        member = jnp.where(mirrored, 15 - block, block)
        place = 2 * ((member - rank) & 3) + ((member // 4) ^ (rank // 4))
        return 2 * place + mirrored.astype(jnp.int32)

    def step(q_ref, block, diagonal):
        slot = slot_of(block)
        both = kv[slot]
        scores = lax.dot_general(
            q_ref[...], both, (((1,), (1,)), ((), ())), preferred_element_type=jnp.float32
        )
        rows = bias[slot]
        scores = scores + jnp.concatenate([rows[0:1], rows[1:2], rows[2:3]], axis=1)
        drops = jnp.maximum(scores, 0.0) + jnp.log(1.0 + jnp.exp(-jnp.abs(scores)))
        if diagonal:
            earlier = lax.broadcasted_iota(jnp.int32, (BLOCK, BLOCK), 1) < lax.broadcasted_iota(
                jnp.int32, (BLOCK, BLOCK), 0
            )
            drops = jnp.where(earlier, drops, 0.0)
        sums = jnp.dot(drops.astype(jnp.bfloat16), later[...], preferred_element_type=jnp.float32)
        within = jnp.exp(scores - sums[:, :BLOCK])
        if diagonal:
            within = jnp.where(earlier, within, 0.0)
        part = jnp.dot(within.astype(jnp.bfloat16), both, preferred_element_type=jnp.float32)
        if diagonal:
            acc[...] = part
            total[...] = sums[:, BLOCK:]
        else:
            acc[...] += jnp.exp(-total[...]) * part
            total[...] += sums[:, BLOCK:]

    for side, q_ref in enumerate((q_own, q_other)):
        last = rank if side == 0 else 15 - rank
        step(q_ref, last, True)

        def body(i, carry):
            step(q_ref, last - 1 - i, False)
            return carry

        lax.fori_loop(0, last, body, 0)
        mixture = acc[:, HEAD:]
        out_ref[pl.ds(side * BLOCK, BLOCK), :] = (rms_scaled(mixture) * gain_ref[...]).astype(
            jnp.bfloat16
        )


def attention(rank, q_own, q_other, pieces, gain):
    vmem = pl.BlockSpec(memory_space=pltpu.VMEM)
    return pl.pallas_call(
        attention_kernel,
        out_shape=jax.ShapeDtypeStruct((2 * BLOCK, HEAD), jnp.bfloat16),
        in_specs=[pl.BlockSpec(memory_space=pltpu.SMEM)] + [vmem] * 11,
        out_specs=vmem,
        scratch_shapes=[
            pltpu.VMEM((16, BLOCK, 128), jnp.bfloat16),
            pltpu.VMEM((16, 16, 128), jnp.float32),
            pltpu.VMEM((BLOCK, BLOCK + 128), jnp.bfloat16),
            pltpu.VMEM((BLOCK, 128), jnp.float32),
            pltpu.VMEM((BLOCK, 128), jnp.float32),
        ],
        compiler_params=pltpu.CompilerParams(vmem_limit_bytes=40 * 1024 * 1024),
        name="attention",
    )(rank, q_own, q_other, *pieces, gain)


def projection_kernel(place_ref, merged, *rest):
    weights, (mine, theirs, acc) = rest[:9], rest[9:]
    z = place_ref[0]
    core = place_ref[1]
    total = None
    for k in range(-3, 4):
        part = jnp.dot(
            merged[(z + k) & 7], weights[k + 3][...], preferred_element_type=jnp.float32
        )
        total = part if total is None else total + part
    far = merged[(z + 4) & 7]
    total = total + jnp.dot(far[:, :64], weights[7][...], preferred_element_type=jnp.float32)
    total = total + jnp.dot(far[:, 64:], weights[8][...], preferred_element_type=jnp.float32)
    acc[...] = total
    rows = mine.shape[0]
    mine[...] = acc[pl.ds(pl.multiple_of(core * rows, 8), rows), :]
    theirs[...] = acc[pl.ds(pl.multiple_of((1 - core) * rows, 8), rows), :]


def projection(place, merged, weights):
    vmem = pl.BlockSpec(memory_space=pltpu.VMEM)
    rows, width = merged.shape[1], weights[0].shape[1]
    half = jax.ShapeDtypeStruct((rows // 2, width), jnp.float32)
    return pl.pallas_call(
        projection_kernel,
        out_shape=(half, half),
        in_specs=[pl.BlockSpec(memory_space=pltpu.SMEM)] + [vmem] * 10,
        out_specs=(vmem, vmem),
        scratch_shapes=[pltpu.VMEM((rows, width), jnp.float32)],
        compiler_params=pltpu.CompilerParams(vmem_limit_bytes=24 * 1024 * 1024),
        name="projection",
    )(place, merged, *weights)


def ring_gather(own):
    half = own.shape[0] // 2
    ahead, behind = [own], [own]
    for _ in range(3):
        behind.append(lax.ppermute(behind[-1], "tp", Z_NEXT))
        ahead.append(lax.ppermute(ahead[-1], "tp", Z_BACK))
    far_low = lax.ppermute(behind[3][:half], "tp", Z_NEXT)
    far_high = lax.ppermute(ahead[3][half:], "tp", Z_BACK)
    return behind, ahead, far_low, far_high


def added(first, second):
    return (first.astype(jnp.float32) + second.astype(jnp.float32)).astype(jnp.bfloat16)


def expert_rows(rows, weights):
    total = None
    for gate_matrix, up_matrix, down_matrix in weights:
        gate_part = jnp.dot(rows, gate_matrix, preferred_element_type=jnp.float32)
        up_part = jnp.dot(rows, up_matrix, preferred_element_type=jnp.float32)
        hidden = (jax.nn.silu(gate_part) * up_part).astype(jnp.bfloat16)
        part = jnp.dot(hidden, down_matrix, preferred_element_type=jnp.float32)
        total = part if total is None else total + part
    return total.astype(jnp.bfloat16)


def on_device(
    queries,
    keys,
    values,
    key_bias,
    head_gain,
    out_weight,
    residual,
    norm_gain,
    gate_proj,
    up_proj,
    down_proj,
    expert_choice,
    expert_weights,
):
    rank = lax.axis_index("sp")
    place = lax.axis_index("tp")
    z, core = place // 2, place % 2
    first_half = rank < 8

    def message(head):
        q = queries[:, head * HEAD : (head + 1) * HEAD] * jnp.bfloat16(HEAD**-0.5)
        q = jnp.concatenate([q, jnp.zeros_like(q)], axis=1)
        k = keys[:, head * HEAD : (head + 1) * HEAD]
        v = values[:, head * HEAD : (head + 1) * HEAD]
        bias_rows = jnp.pad(key_bias[:, head].reshape(3, 128), ((0, 13), (0, 0)))
        return jnp.concatenate([jnp.concatenate([k, v], axis=1), bias_rows, q], axis=0)

    even, odd = message(0), message(1)
    kept = jnp.where(first_half, even, odd)
    swapped = lax.ppermute(jnp.where(first_half, odd, even), "sp", PARTNER)
    own = jnp.concatenate([kept[:PIECE], swapped[:PIECE]], axis=0)

    across = lax.ppermute(own, "sp", Y_SWAP)
    from_back = lax.ppermute(own, "sp", X_NEXT)
    from_next = lax.ppermute(own, "sp", X_BACK)
    across_back = lax.ppermute(across, "sp", X_NEXT)
    across_next = lax.ppermute(across, "sp", X_BACK)
    opposite = lax.ppermute(from_back, "sp", X_NEXT)
    across_opposite = lax.ppermute(across_next, "sp", X_BACK)
    pieces = (
        own,
        across,
        from_next,
        across_next,
        opposite,
        across_opposite,
        from_back,
        across_back,
    )

    weights_own = (gate_proj[0], up_proj[0], down_proj[0])
    weights_other = tuple(lax.ppermute(w, "tp", CORE_SWAP) for w in weights_own)
    behind, ahead, far_low, far_high = ring_gather(out_weight)

    gain = jnp.where(first_half, head_gain[0:1], head_gain[1:2])
    attended = attention(rank.reshape(1), kept[PIECE:], swapped[PIECE:], pieces, gain)
    returned_head = lax.ppermute(attended[BLOCK:], "sp", PARTNER)
    kept_head = attended[:BLOCK]
    both_heads = jnp.where(
        first_half,
        jnp.concatenate([kept_head, returned_head], axis=1),
        jnp.concatenate([returned_head, kept_head], axis=1),
    )
    merged = lax.all_to_all(
        both_heads.reshape(RING, BLOCK // RING, 2 * HEAD),
        "tp",
        split_axis=0,
        concat_axis=0,
        axis_index_groups=SAME_CORE,
        tiled=True,
    )
    mine, theirs = projection(
        jnp.stack([z, core]),
        merged,
        [behind[3], behind[2], behind[1], out_weight, ahead[1], ahead[2], ahead[3]]
        + [far_low, far_high],
    )
    projected = mine + lax.ppermute(theirs, "tp", CORE_SWAP)
    stream = (residual.astype(jnp.float32) + projected).astype(jnp.bfloat16)
    normed = (rms_scaled(stream.astype(jnp.float32)) * norm_gain).astype(jnp.bfloat16)

    experts_all = lax.axis_size("sp")
    row_share, model_width = residual.shape
    capacity = row_share // 4
    own_slots = expert_choice * capacity + choice_ranks(expert_choice, experts_all)
    wanted = slot_tokens(own_slots, experts_all * capacity, row_share)
    outgoing = jnp.take(normed, wanted, axis=0, mode="fill", fill_value=0)
    arrived = lax.all_to_all(outgoing, "sp", split_axis=0, concat_axis=0, tiled=True)

    weights = (weights_own, weights_other)
    count = experts_all * capacity
    half = count // 2
    rows_behind, rows_ahead, rows_low, rows_high = ring_gather(arrived)

    def pair_rows(first, second):
        out = expert_rows(jnp.concatenate([first, second], axis=0), weights)
        return out[: first.shape[0]], out[first.shape[0] :]

    part_own = expert_rows(arrived, weights)
    part_behind, part_ahead = {}, {}
    for k in range(1, 4):
        part_behind[k], part_ahead[k] = pair_rows(rows_behind[k], rows_ahead[k])
    part_low, part_high = pair_rows(rows_low, rows_high)

    forward = lax.ppermute(part_low, "tp", Z_NEXT)
    backward = lax.ppermute(part_high, "tp", Z_BACK)
    forward = jnp.concatenate([added(forward, part_ahead[3][:half]), part_ahead[3][half:]], axis=0)
    backward = jnp.concatenate(
        [part_behind[3][:half], added(backward, part_behind[3][half:])], axis=0
    )
    for k in (2, 1):
        forward = added(lax.ppermute(forward, "tp", Z_NEXT), part_ahead[k])
        backward = added(lax.ppermute(backward, "tp", Z_BACK), part_behind[k])
    forward = lax.ppermute(forward, "tp", Z_NEXT)
    backward = lax.ppermute(backward, "tp", Z_BACK)
    summed = (
        forward.astype(jnp.float32)
        + backward.astype(jnp.float32)
        + part_own.astype(jnp.float32)
    ).astype(jnp.bfloat16)

    returned = lax.all_to_all(summed, "sp", split_axis=0, concat_axis=0, tiled=True)
    picked = jnp.take(returned, own_slots, axis=0).astype(jnp.float32)
    combined = jnp.sum(expert_weights[:, :, None] * picked, axis=1)
    return (stream.astype(jnp.float32) + combined).astype(jnp.bfloat16)


def solution(mesh):
    placed = (
        P("sp", "tp"),
        P("sp", "tp"),
        P("sp", "tp"),
        P("sp", "tp"),
        P("tp", None),
        P("tp", None),
        P(("sp", "tp"), None),
        P(),
        P("sp", None, "tp"),
        P("sp", None, "tp"),
        P("sp", "tp", None),
        P(("sp", "tp"), None),
        P(("sp", "tp"), None),
    )
    return jax.shard_map(
        on_device, mesh=mesh, in_specs=placed, out_specs=P(("sp", "tp"), None), check_vma=False
    )
```

```python
import jax
import jax.numpy as jnp
from jax import lax
from jax.experimental import pallas as pl
from jax.experimental.pallas import tpu as pltpu
from jax.sharding import PartitionSpec as P

epsilon = 1e-06
BLOCK = 384
HEAD = 64
PIECE = BLOCK + 16
RING = 8

PARTNER = [(i, 15 - i) for i in range(16)]
Y_SWAP = [(i, i ^ 4) for i in range(16)]
X_NEXT = [(i, i // 4 * 4 + (i + 1) % 4) for i in range(16)]
X_BACK = [(i, i // 4 * 4 + (i + 3) % 4) for i in range(16)]
Z_NEXT = [(i, (i + 2) % 16) for i in range(16)]
Z_BACK = [(i, (i + 14) % 16) for i in range(16)]
CORE_SWAP = [(i, i ^ 1) for i in range(16)]


def rms_scaled(values_in):
    return values_in * lax.rsqrt(jnp.mean(values_in * values_in, axis=-1, keepdims=True) + epsilon)


def choice_ranks(routes, experts_all):
    flat_routes = routes.reshape(routes.shape[:-2] + (-1,))
    onehot = (flat_routes[..., None] == jnp.arange(experts_all, dtype=jnp.int32)).astype(jnp.int32)
    before = jnp.cumsum(onehot, axis=-2) - onehot
    return jnp.sum(before * onehot, axis=-1).reshape(routes.shape)


def slot_tokens(slot_index, targets, missing):
    flat_slots = slot_index.reshape(-1)
    owners = jnp.arange(flat_slots.shape[0], dtype=jnp.int32) // 2
    matches = flat_slots[None, :] == jnp.arange(targets, dtype=jnp.int32)[:, None]
    owner_found = jnp.sum(jnp.where(matches, owners[None, :], 0), axis=1)
    return jnp.where(jnp.any(matches, axis=1), owner_found, missing)


def attention_kernel(rank_ref, q_own, q_other, *rest):
    pieces, (gain_ref, out_ref, kv, bias, later, acc, total, q) = rest[:8], rest[8:]
    rank = rank_ref[0]
    q[0] = q_own[...]
    q[1] = q_other[...]
    for j in range(8):
        for half in range(2):
            start = half * PIECE
            kv[2 * j + half] = pieces[j][start : start + BLOCK, :]
            bias[2 * j + half] = pieces[j][start + BLOCK : start + PIECE, :].astype(jnp.float32)
    row = lax.broadcasted_iota(jnp.int32, (BLOCK, BLOCK + 128), 0)
    col = lax.broadcasted_iota(jnp.int32, (BLOCK, BLOCK + 128), 1)
    later[...] = jnp.where((row >= col) | (col >= BLOCK), 1.0, 0.0).astype(jnp.bfloat16)

    def slot_of(block):
        mirrored = (block // 8) != (rank // 8)
        member = jnp.where(mirrored, 15 - block, block)
        place = 2 * ((member - rank) & 3) + ((member // 4) ^ (rank // 4))
        return 2 * place + mirrored.astype(jnp.int32)

    def step(side, block, diagonal):
        slot = slot_of(block)
        both = kv[slot]
        scores = lax.dot_general(
            q[side], both, (((1,), (1,)), ((), ())), preferred_element_type=jnp.float32
        )
        rows = bias[slot]
        scores = scores + jnp.concatenate([rows[0:1], rows[1:2], rows[2:3]], axis=1)
        drops = jnp.maximum(scores, 0.0) + jnp.log(1.0 + jnp.exp(-jnp.abs(scores)))
        if diagonal:
            earlier = lax.broadcasted_iota(jnp.int32, (BLOCK, BLOCK), 1) < lax.broadcasted_iota(
                jnp.int32, (BLOCK, BLOCK), 0
            )
            drops = jnp.where(earlier, drops, 0.0)
        sums = jnp.dot(drops.astype(jnp.bfloat16), later[...], preferred_element_type=jnp.float32)
        within = jnp.exp(scores - sums[:, :BLOCK])
        if diagonal:
            within = jnp.where(earlier, within, 0.0)
        part = jnp.dot(within.astype(jnp.bfloat16), both, preferred_element_type=jnp.float32)
        if diagonal:
            acc[...] = part
            total[...] = sums[:, BLOCK:]
        else:
            acc[...] += jnp.exp(-total[...]) * part
            total[...] += sums[:, BLOCK:]

    def one_side(side, carry):
        last = jnp.where(side == 0, rank, 15 - rank)
        step(side, last, True)

        def body(i, carry):
            step(side, last - 1 - i, False)
            return carry

        lax.fori_loop(0, last, body, 0)
        mixture = acc[:, HEAD:]
        rows = pl.ds(pl.multiple_of(side * BLOCK, BLOCK), BLOCK)
        out_ref[rows, :] = (rms_scaled(mixture) * gain_ref[...]).astype(jnp.bfloat16)
        return carry

    lax.fori_loop(0, 2, one_side, 0)


def attention(rank, q_own, q_other, pieces, gain):
    vmem = pl.BlockSpec(memory_space=pltpu.VMEM)
    return pl.pallas_call(
        attention_kernel,
        out_shape=jax.ShapeDtypeStruct((2 * BLOCK, HEAD), jnp.bfloat16),
        in_specs=[pl.BlockSpec(memory_space=pltpu.SMEM)] + [vmem] * 11,
        out_specs=vmem,
        scratch_shapes=[
            pltpu.VMEM((16, BLOCK, 128), jnp.bfloat16),
            pltpu.VMEM((16, 16, 128), jnp.float32),
            pltpu.VMEM((BLOCK, BLOCK + 128), jnp.bfloat16),
            pltpu.VMEM((BLOCK, 128), jnp.float32),
            pltpu.VMEM((BLOCK, 128), jnp.float32),
            pltpu.VMEM((2, BLOCK, 128), jnp.bfloat16),
        ],
        compiler_params=pltpu.CompilerParams(vmem_limit_bytes=16 * 1024 * 1024),
        cost_estimate=pl.CostEstimate(
            flops=34 * BLOCK * BLOCK * (BLOCK + 384), bytes_accessed=1 << 21, transcendentals=0
        ),
        name="attention",
    )(rank, q_own, q_other, *pieces, gain)


def projection_kernel(place_ref, own_head, other_head, weight, mine, theirs, full):
    core = place_ref[1]
    kept_first = place_ref[0] == 1
    a, b = own_head[...], other_head[...]
    low = jnp.where(kept_first, a, b)
    high = jnp.where(kept_first, b, a)
    both = jnp.concatenate([low, high], axis=1)
    full[...] = jnp.dot(both, weight[...], preferred_element_type=jnp.float32)
    rows = mine.shape[1]
    for chip in range(RING):
        at = 2 * chip * rows
        mine[chip] = full[pl.ds(pl.multiple_of(at + core * rows, 8), rows), :].astype(jnp.bfloat16)
        theirs[chip] = full[pl.ds(pl.multiple_of(at + (1 - core) * rows, 8), rows), :].astype(
            jnp.bfloat16
        )


def projection(flags, own_head, other_head, weight):
    vmem = pl.BlockSpec(memory_space=pltpu.VMEM)
    rows, width = own_head.shape[0], weight.shape[1]
    half = jax.ShapeDtypeStruct((RING, rows // (2 * RING), width), jnp.bfloat16)
    return pl.pallas_call(
        projection_kernel,
        out_shape=(half, half),
        in_specs=[pl.BlockSpec(memory_space=pltpu.SMEM)] + [vmem] * 3,
        out_specs=(vmem, vmem),
        scratch_shapes=[pltpu.VMEM((rows, width), jnp.float32)],
        compiler_params=pltpu.CompilerParams(vmem_limit_bytes=16 * 1024 * 1024),
        name="projection",
    )(flags, own_head, other_head, weight)


def ring_gather(own):
    half = own.shape[0] // 2
    ahead, behind = [own], [own]
    for _ in range(3):
        behind.append(lax.ppermute(behind[-1], "tp", Z_NEXT))
        ahead.append(lax.ppermute(ahead[-1], "tp", Z_BACK))
    far_low = lax.ppermute(behind[3][:half], "tp", Z_NEXT)
    far_high = lax.ppermute(ahead[3][half:], "tp", Z_BACK)
    return behind, ahead, far_low, far_high


def added(first, second):
    return (first.astype(jnp.float32) + second.astype(jnp.float32)).astype(jnp.bfloat16)


def expert_kernel(count, *refs):
    rows, weights, outs, gathered = refs[:count], refs[count : count + 6], refs[count + 6 : -1], refs[-1]
    at = 0
    for piece in rows:
        gathered[pl.ds(at, piece.shape[0]), :] = piece[...]
        at += piece.shape[0]
    total = None
    for gate_matrix, up_matrix, down_matrix in (weights[:3], weights[3:]):
        across = (((1,), (1,)), ((), ()))
        gate_part = lax.dot_general(
            gathered[...], gate_matrix[...], across, preferred_element_type=jnp.float32
        )
        up_part = lax.dot_general(
            gathered[...], up_matrix[...], across, preferred_element_type=jnp.float32
        )
        hidden = (gate_part / (1.0 + jnp.exp(-gate_part)) * up_part).astype(jnp.bfloat16)
        part = jnp.dot(hidden, down_matrix[...], preferred_element_type=jnp.float32)
        total = part if total is None else total + part
    total = total.astype(jnp.bfloat16)
    at = 0
    for out in outs:
        out[...] = total[at : at + out.shape[0]]
        at += out.shape[0]


def expert_rows(rows, weights, halves):
    vmem = pl.BlockSpec(memory_space=pltpu.VMEM)
    count = sum(piece.shape[0] for piece in rows)
    width = rows[0].shape[1]
    shapes = []
    for piece in rows:
        n = piece.shape[0]
        shapes += [(n // 2, width)] * 2 if halves and n % 32 == 0 else [(n, width)]
    return pl.pallas_call(
        lambda *refs: expert_kernel(len(rows), *refs),
        out_shape=[jax.ShapeDtypeStruct(shape, jnp.bfloat16) for shape in shapes],
        in_specs=[vmem] * (len(rows) + 6),
        out_specs=[vmem] * len(shapes),
        scratch_shapes=[pltpu.VMEM((count, width), jnp.bfloat16)],
        compiler_params=pltpu.CompilerParams(vmem_limit_bytes=28 * 1024 * 1024),
        cost_estimate=pl.CostEstimate(
            flops=12 * count * width * weights[0].shape[0],
            bytes_accessed=12 * width * weights[0].shape[0],
            transcendentals=2 * count * weights[0].shape[0],
        ),
        name="expert",
    )(*rows, *weights)


def on_device(
    queries,
    keys,
    values,
    key_bias,
    head_gain,
    out_weight,
    residual,
    norm_gain,
    gate_proj,
    up_proj,
    down_proj,
    expert_choice,
    expert_weights,
):
    rank = lax.axis_index("sp")
    place = lax.axis_index("tp")
    z, core = place // 2, place % 2
    first_half = rank < 8

    def message(head):
        q = queries[:, head * HEAD : (head + 1) * HEAD] * jnp.bfloat16(HEAD**-0.5)
        q = jnp.concatenate([q, jnp.zeros_like(q)], axis=1)
        k = keys[:, head * HEAD : (head + 1) * HEAD]
        v = values[:, head * HEAD : (head + 1) * HEAD]
        bias_rows = jnp.pad(key_bias[:, head].reshape(3, 128), ((0, 13), (0, 0)))
        return jnp.concatenate([jnp.concatenate([k, v], axis=1), bias_rows, q], axis=0)

    even, odd = message(0), message(1)
    kept = jnp.where(first_half, even, odd)
    swapped = lax.ppermute(jnp.where(first_half, odd, even), "sp", PARTNER)
    own = jnp.concatenate([kept[:PIECE], swapped[:PIECE]], axis=0)

    across = lax.ppermute(own, "sp", Y_SWAP)
    from_back = lax.ppermute(own, "sp", X_NEXT)
    from_next = lax.ppermute(own, "sp", X_BACK)
    across_back = lax.ppermute(across, "sp", X_NEXT)
    across_next = lax.ppermute(across, "sp", X_BACK)
    opposite = lax.ppermute(from_back, "sp", X_NEXT)
    across_opposite = lax.ppermute(across_next, "sp", X_BACK)
    pieces = (
        own,
        across,
        from_next,
        across_next,
        opposite,
        across_opposite,
        from_back,
        across_back,
    )

    gain = jnp.where(first_half, head_gain[0:1], head_gain[1:2])
    weights_own = (gate_proj[0].T, up_proj[0].T, down_proj[0])
    pieces, weights_out = lax.optimization_barrier((pieces, weights_own))
    weights_other = tuple(lax.ppermute(w, "tp", CORE_SWAP) for w in weights_out)
    attended = attention(rank.reshape(1), kept[PIECE:], swapped[PIECE:], pieces, gain)
    attended, weights_other = lax.optimization_barrier((attended, weights_other))
    returned_head = lax.ppermute(attended[BLOCK:], "sp", PARTNER)
    flags = jnp.stack([first_half.astype(jnp.int32), core])
    mine, theirs = projection(flags, attended[:BLOCK], returned_head, out_weight)
    share = added(mine, lax.ppermute(theirs, "tp", CORE_SWAP))

    def share_at(offset):
        return lax.dynamic_index_in_dim(share, (z + offset) & (RING - 1), 0, keepdims=False)

    forward, backward = share_at(4), share_at(-3)
    for k in (3, 2, 1):
        forward = added(lax.ppermute(forward, "tp", Z_NEXT), share_at(k))
        if k < 3:
            backward = added(lax.ppermute(backward, "tp", Z_BACK), share_at(-k))
    forward = lax.ppermute(forward, "tp", Z_NEXT)
    backward = lax.ppermute(backward, "tp", Z_BACK)
    projected = (
        forward.astype(jnp.float32) + backward.astype(jnp.float32) + share_at(0).astype(jnp.float32)
    )
    stream = (residual.astype(jnp.float32) + projected).astype(jnp.bfloat16)
    normed = (rms_scaled(stream.astype(jnp.float32)) * norm_gain).astype(jnp.bfloat16)

    experts_all = lax.axis_size("sp")
    row_share, model_width = residual.shape
    capacity = row_share // 4
    own_slots = expert_choice * capacity + choice_ranks(expert_choice, experts_all)
    wanted = slot_tokens(own_slots, experts_all * capacity, row_share)
    outgoing = jnp.take(normed, wanted, axis=0, mode="fill", fill_value=0)
    arrived = lax.all_to_all(outgoing, "sp", split_axis=0, concat_axis=0, tiled=True)

    weights = (*weights_own, *weights_other)
    half = arrived.shape[0] // 2
    part_behind, part_ahead = {}, {}
    below = lax.ppermute(arrived, "tp", Z_NEXT)
    above = lax.ppermute(arrived, "tp", Z_BACK)
    for k in (1, 2, 3):
        if k < 3:
            next_below = lax.ppermute(below, "tp", Z_NEXT)
            next_above = lax.ppermute(above, "tp", Z_BACK)
        else:
            next_below = lax.ppermute(below[:half], "tp", Z_NEXT)
            next_above = lax.ppermute(above[half:], "tp", Z_BACK)
        rows = (below, above, arrived) if k == 1 else (below, above)
        parts = expert_rows(rows, weights, True)
        next_below, next_above, parts = lax.optimization_barrier((next_below, next_above, parts))
        part_behind[k], part_ahead[k] = parts[0:2], parts[2:4]
        if k == 1:
            part_own = parts[4:6]
        below, above = next_below, next_above
    part_low, part_high = expert_rows((below, above), weights, False)

    summed = []
    for side, far in ((0, part_low), (1, part_high)):
        long_way, back_way = (Z_NEXT, Z_BACK) if side == 0 else (Z_BACK, Z_NEXT)
        long_parts, back_parts = (
            (part_ahead, part_behind) if side == 0 else (part_behind, part_ahead)
        )
        total, other = lax.ppermute(far, "tp", long_way), back_parts[3][side]
        for k in (3, 2, 1):
            total = lax.ppermute(added(total, long_parts[k][side]), "tp", long_way)
        for k in (2, 1):
            other = added(lax.ppermute(other, "tp", back_way), back_parts[k][side])
        other = lax.ppermute(other, "tp", back_way)
        summed.append(
            (
                total.astype(jnp.float32)
                + other.astype(jnp.float32)
                + part_own[side].astype(jnp.float32)
            ).astype(jnp.bfloat16)
        )
    summed = jnp.concatenate(summed, axis=0)

    returned = lax.all_to_all(summed, "sp", split_axis=0, concat_axis=0, tiled=True)
    picked = jnp.take(returned, own_slots, axis=0).astype(jnp.float32)
    combined = jnp.sum(expert_weights[:, :, None] * picked, axis=1)
    return (stream.astype(jnp.float32) + combined).astype(jnp.bfloat16)


def solution(mesh):
    placed = (
        P("sp", "tp"),
        P("sp", "tp"),
        P("sp", "tp"),
        P("sp", "tp"),
        P("tp", None),
        P("tp", None),
        P(("sp", "tp"), None),
        P(),
        P("sp", None, "tp"),
        P("sp", None, "tp"),
        P("sp", "tp", None),
        P(("sp", "tp"), None),
        P(("sp", "tp"), None),
    )
    return jax.shard_map(
        on_device, mesh=mesh, in_specs=placed, out_specs=P(("sp", "tp"), None), check_vma=False
    )
```

```python
import jax
import jax.numpy as jnp
from jax import lax
from jax.experimental import pallas as pl
from jax.experimental.pallas import tpu as pltpu
from jax.sharding import PartitionSpec as P


epsilon = 1e-06
BLOCK = 384
HEAD = 64
PIECE = BLOCK + 16
RING = 8

PARTNER = [(i, 15 - i) for i in range(16)]
Y_SWAP = [(i, i ^ 4) for i in range(16)]
X_NEXT = [(i, i // 4 * 4 + (i + 1) % 4) for i in range(16)]
X_BACK = [(i, i // 4 * 4 + (i + 3) % 4) for i in range(16)]
Z_NEXT = [(i, (i + 2) % 16) for i in range(16)]
Z_BACK = [(i, (i + 14) % 16) for i in range(16)]
Z_FAR = [(i, (i + 8) % 16) for i in range(16)]
CORE_SWAP = [(i, i ^ 1) for i in range(16)]


def rms_scaled(values_in):
    return values_in * lax.rsqrt(jnp.mean(values_in * values_in, axis=-1, keepdims=True) + epsilon)


def choice_ranks(routes, experts_all):
    flat_routes = routes.reshape(routes.shape[:-2] + (-1,))
    onehot = (flat_routes[..., None] == jnp.arange(experts_all, dtype=jnp.int32)).astype(jnp.int32)
    before = jnp.cumsum(onehot, axis=-2) - onehot
    return jnp.sum(before * onehot, axis=-1).reshape(routes.shape)


def slot_tokens(slot_index, targets, missing):
    flat_slots = slot_index.reshape(-1)
    owners = jnp.arange(flat_slots.shape[0], dtype=jnp.int32) // 2
    matches = flat_slots[None, :] == jnp.arange(targets, dtype=jnp.int32)[:, None]
    owner_found = jnp.sum(jnp.where(matches, owners[None, :], 0), axis=1)
    return jnp.where(jnp.any(matches, axis=1), owner_found, missing)


def attention_kernel(rank_ref, q_own, q_other, *rest):
    pieces, (gain_ref, out_ref, kv, bias, later, acc, total, q) = rest[:8], rest[8:]
    rank = rank_ref[0]
    q[0] = q_own[...]
    q[1] = q_other[...]
    for j in range(8):
        for half in range(2):
            start = half * PIECE
            kv[2 * j + half] = pieces[j][start : start + BLOCK, :]
            bias[2 * j + half] = pieces[j][start + BLOCK : start + PIECE, :].astype(jnp.float32)
    row = lax.broadcasted_iota(jnp.int32, (BLOCK, BLOCK + 128), 0)
    col = lax.broadcasted_iota(jnp.int32, (BLOCK, BLOCK + 128), 1)
    later[...] = jnp.where((row >= col) | (col >= BLOCK), 1.0, 0.0).astype(jnp.bfloat16)

    def slot_of(block):
        mirrored = (block // 8) != (rank // 8)
        member = jnp.where(mirrored, 15 - block, block)
        place = 2 * ((member - rank) & 3) + ((member // 4) ^ (rank // 4))
        return 2 * place + mirrored.astype(jnp.int32)

    def step(side, block, diagonal):
        slot = slot_of(block)
        both = kv[slot]
        scores = lax.dot_general(
            q[side], both, (((1,), (1,)), ((), ())), preferred_element_type=jnp.float32
        )
        rows = bias[slot]
        scores = scores + jnp.concatenate([rows[0:1], rows[1:2], rows[2:3]], axis=1)
        drops = jnp.maximum(scores, 0.0) + jnp.log(1.0 + jnp.exp(-jnp.abs(scores)))
        if diagonal:
            earlier = lax.broadcasted_iota(jnp.int32, (BLOCK, BLOCK), 1) < lax.broadcasted_iota(
                jnp.int32, (BLOCK, BLOCK), 0
            )
            drops = jnp.where(earlier, drops, 0.0)
        sums = jnp.dot(drops.astype(jnp.bfloat16), later[...], preferred_element_type=jnp.float32)
        within = jnp.exp(scores - sums[:, :BLOCK])
        if diagonal:
            within = jnp.where(earlier, within, 0.0)
        part = jnp.dot(within.astype(jnp.bfloat16), both, preferred_element_type=jnp.float32)
        if diagonal:
            acc[...] = part
            total[...] = sums[:, BLOCK:]
        else:
            acc[...] += jnp.exp(-total[...]) * part
            total[...] += sums[:, BLOCK:]

    def one_side(side, carry):
        last = jnp.where(side == 0, rank, 15 - rank)
        step(side, last, True)

        def body(i, carry):
            step(side, last - 1 - i, False)
            return carry

        lax.fori_loop(0, last, body, 0)
        mixture = acc[:, HEAD:]
        rows = pl.ds(pl.multiple_of(side * BLOCK, BLOCK), BLOCK)
        out_ref[rows, :] = (rms_scaled(mixture) * gain_ref[...]).astype(jnp.bfloat16)
        return carry

    lax.fori_loop(0, 2, one_side, 0)


def attention(rank, q_own, q_other, pieces, gain):
    vmem = pl.BlockSpec(memory_space=pltpu.VMEM)
    return pl.pallas_call(
        attention_kernel,
        out_shape=jax.ShapeDtypeStruct((2 * BLOCK, HEAD), jnp.bfloat16),
        in_specs=[pl.BlockSpec(memory_space=pltpu.SMEM)] + [vmem] * 11,
        out_specs=vmem,
        scratch_shapes=[
            pltpu.VMEM((16, BLOCK, 128), jnp.bfloat16),
            pltpu.VMEM((16, 16, 128), jnp.float32),
            pltpu.VMEM((BLOCK, BLOCK + 128), jnp.bfloat16),
            pltpu.VMEM((BLOCK, 128), jnp.float32),
            pltpu.VMEM((BLOCK, 128), jnp.float32),
            pltpu.VMEM((2, BLOCK, 128), jnp.bfloat16),
        ],
        compiler_params=pltpu.CompilerParams(vmem_limit_bytes=16 * 1024 * 1024),
        cost_estimate=pl.CostEstimate(
            flops=34 * BLOCK * BLOCK * (BLOCK + 384), bytes_accessed=1 << 21, transcendentals=0
        ),
        name="attention",
    )(rank, q_own, q_other, *pieces, gain)


def projection_kernel(place_ref, own_head, other_head, weight, mine, theirs, full):
    core = place_ref[1]
    kept_first = place_ref[0] == 1
    a, b = own_head[...], other_head[...]
    low = jnp.where(kept_first, a, b)
    high = jnp.where(kept_first, b, a)
    both = jnp.concatenate([low, high], axis=1)
    full[...] = jnp.dot(both, weight[...], preferred_element_type=jnp.float32)
    rows = mine.shape[1]
    for chip in range(RING):
        at = 2 * chip * rows
        mine[chip] = full[pl.ds(pl.multiple_of(at + core * rows, 8), rows), :].astype(jnp.bfloat16)
        theirs[chip] = full[pl.ds(pl.multiple_of(at + (1 - core) * rows, 8), rows), :].astype(
            jnp.bfloat16
        )


def projection(flags, own_head, other_head, weight):
    vmem = pl.BlockSpec(memory_space=pltpu.VMEM)
    rows, width = own_head.shape[0], weight.shape[1]
    half = jax.ShapeDtypeStruct((RING, rows // (2 * RING), width), jnp.bfloat16)
    return pl.pallas_call(
        projection_kernel,
        out_shape=(half, half),
        in_specs=[pl.BlockSpec(memory_space=pltpu.SMEM)] + [vmem] * 3,
        out_specs=(vmem, vmem),
        scratch_shapes=[pltpu.VMEM((rows, width), jnp.float32)],
        compiler_params=pltpu.CompilerParams(vmem_limit_bytes=16 * 1024 * 1024),
        name="projection",
    )(flags, own_head, other_head, weight)


def added(first, second):
    return (first.astype(jnp.float32) + second.astype(jnp.float32)).astype(jnp.bfloat16)


def expert_kernel(count, *refs):
    rows, weights, outs, gathered = refs[:count], refs[count : count + 6], refs[count + 6 : -1], refs[-1]
    at = 0
    for piece in rows:
        gathered[pl.ds(at, piece.shape[0]), :] = piece[...]
        at += piece.shape[0]
    total = None
    for gate_matrix, up_matrix, down_matrix in (weights[:3], weights[3:]):
        across = (((1,), (1,)), ((), ()))
        gate_part = lax.dot_general(
            gathered[...], gate_matrix[...], across, preferred_element_type=jnp.float32
        )
        up_part = lax.dot_general(
            gathered[...], up_matrix[...], across, preferred_element_type=jnp.float32
        )
        hidden = (gate_part / (1.0 + jnp.exp(-gate_part)) * up_part).astype(jnp.bfloat16)
        part = jnp.dot(hidden, down_matrix[...], preferred_element_type=jnp.float32)
        total = part if total is None else total + part
    total = total.astype(jnp.bfloat16)
    at = 0
    for out in outs:
        out[...] = total[at : at + out.shape[0]]
        at += out.shape[0]


def expert_rows(rows, weights):
    vmem = pl.BlockSpec(memory_space=pltpu.VMEM)
    count = sum(piece.shape[0] for piece in rows)
    width = rows[0].shape[1]
    shapes = []
    for piece in rows:
        n = piece.shape[0]
        shapes += [(n // 2, width)] * 2
    return pl.pallas_call(
        lambda *refs: expert_kernel(len(rows), *refs),
        out_shape=[jax.ShapeDtypeStruct(shape, jnp.bfloat16) for shape in shapes],
        in_specs=[vmem] * (len(rows) + 6),
        out_specs=[vmem] * len(shapes),
        scratch_shapes=[pltpu.VMEM((count, width), jnp.bfloat16)],
        compiler_params=pltpu.CompilerParams(vmem_limit_bytes=28 * 1024 * 1024),
        cost_estimate=pl.CostEstimate(
            flops=12 * count * width * weights[0].shape[0],
            bytes_accessed=12 * width * weights[0].shape[0],
            transcendentals=2 * count * weights[0].shape[0],
        ),
        name="expert",
    )(*rows, *weights)


def on_device(
    queries,
    keys,
    values,
    key_bias,
    head_gain,
    out_weight,
    residual,
    norm_gain,
    gate_proj,
    up_proj,
    down_proj,
    expert_choice,
    expert_weights,
):
    rank = lax.axis_index("sp")
    place = lax.axis_index("tp")
    z, core = place // 2, place % 2
    first_half = rank < 8

    def message(head):
        q = queries[:, head * HEAD : (head + 1) * HEAD] * jnp.bfloat16(HEAD**-0.5)
        q = jnp.concatenate([q, jnp.zeros_like(q)], axis=1)
        k = keys[:, head * HEAD : (head + 1) * HEAD]
        v = values[:, head * HEAD : (head + 1) * HEAD]
        bias_rows = jnp.pad(key_bias[:, head].reshape(3, 128), ((0, 13), (0, 0)))
        return jnp.concatenate([jnp.concatenate([k, v], axis=1), bias_rows, q], axis=0)

    even, odd = message(0), message(1)
    kept = jnp.where(first_half, even, odd)
    swapped = lax.ppermute(jnp.where(first_half, odd, even), "sp", PARTNER)
    own = jnp.concatenate([kept[:PIECE], swapped[:PIECE]], axis=0)

    across = lax.ppermute(own, "sp", Y_SWAP)
    from_back = lax.ppermute(own, "sp", X_NEXT)
    from_next = lax.ppermute(own, "sp", X_BACK)
    across_back = lax.ppermute(across, "sp", X_NEXT)
    across_next = lax.ppermute(across, "sp", X_BACK)
    opposite = lax.ppermute(from_back, "sp", X_NEXT)
    across_opposite = lax.ppermute(across_next, "sp", X_BACK)
    pieces = (
        own,
        across,
        from_next,
        across_next,
        opposite,
        across_opposite,
        from_back,
        across_back,
    )

    gain = jnp.where(first_half, head_gain[0:1], head_gain[1:2])
    weights_own = (gate_proj[0].T, up_proj[0].T, down_proj[0])
    pieces, weights_out = lax.optimization_barrier((pieces, weights_own))
    weights_other = tuple(lax.ppermute(w, "tp", CORE_SWAP) for w in weights_out)
    attended = attention(rank.reshape(1), kept[PIECE:], swapped[PIECE:], pieces, gain)
    attended, weights_other = lax.optimization_barrier((attended, weights_other))
    returned_head = lax.ppermute(attended[BLOCK:], "sp", PARTNER)
    flags = jnp.stack([first_half.astype(jnp.int32), core])
    mine, theirs = projection(flags, attended[:BLOCK], returned_head, out_weight)
    share = added(mine, lax.ppermute(theirs, "tp", CORE_SWAP))

    def share_at(offset):
        return lax.dynamic_index_in_dim(share, (z + offset) & (RING - 1), 0, keepdims=False)

    far_share = lax.ppermute(share_at(4), "tp", Z_FAR)
    forward, backward = share_at(3), share_at(-3)
    for k in (2, 1):
        forward = added(lax.ppermute(forward, "tp", Z_NEXT), share_at(k))
        backward = added(lax.ppermute(backward, "tp", Z_BACK), share_at(-k))
    forward = lax.ppermute(forward, "tp", Z_NEXT)
    backward = lax.ppermute(backward, "tp", Z_BACK)
    projected = (
        forward.astype(jnp.float32)
        + backward.astype(jnp.float32)
        + far_share.astype(jnp.float32)
        + share_at(0).astype(jnp.float32)
    )
    stream = (residual.astype(jnp.float32) + projected).astype(jnp.bfloat16)
    normed = (rms_scaled(stream.astype(jnp.float32)) * norm_gain).astype(jnp.bfloat16)

    experts_all = lax.axis_size("sp")
    row_share, _ = residual.shape
    capacity = row_share // 4
    own_slots = expert_choice * capacity + choice_ranks(expert_choice, experts_all)
    wanted = slot_tokens(own_slots, experts_all * capacity, row_share)
    outgoing = jnp.take(normed, wanted, axis=0, mode="fill", fill_value=0)
    arrived = lax.all_to_all(outgoing, "sp", split_axis=0, concat_axis=0, tiled=True)

    weights = (*weights_own, *weights_other)
    half = arrived.shape[0] // 2
    part_behind, part_ahead = {}, {}
    below = lax.ppermute(arrived, "tp", Z_NEXT)
    above = lax.ppermute(arrived, "tp", Z_BACK)
    for k in (1, 2, 3):
        if k < 3:
            next_below = lax.ppermute(below, "tp", Z_NEXT)
            next_above = lax.ppermute(above, "tp", Z_BACK)
        else:
            next_below = lax.ppermute(below[:half], "tp", Z_NEXT)
            next_above = lax.ppermute(above[half:], "tp", Z_BACK)
        parts = expert_rows((below, above), weights)
        next_below, next_above, parts = lax.optimization_barrier((next_below, next_above, parts))
        part_behind[k], part_ahead[k] = parts[0:2], parts[2:4]
        below, above = next_below, next_above
    far = jnp.concatenate([below, above], axis=0)
    first_hops = []
    for side in range(2):
        back_way = Z_BACK if side == 0 else Z_NEXT
        back_parts = part_behind if side == 0 else part_ahead
        first_hops.append(lax.ppermute(back_parts[3][side], "tp", back_way))
    part_low, part_high, *part_own = expert_rows((far, arrived), weights)

    summed = []
    for side, far in ((0, part_low), (1, part_high)):
        long_way, back_way = (Z_NEXT, Z_BACK) if side == 0 else (Z_BACK, Z_NEXT)
        long_parts, back_parts = (
            (part_ahead, part_behind) if side == 0 else (part_behind, part_ahead)
        )
        total = lax.ppermute(far, "tp", long_way)
        for k in (3, 2, 1):
            total = lax.ppermute(added(total, long_parts[k][side]), "tp", long_way)
        for k in (2, 1):
            other = first_hops[side] if k == 2 else lax.ppermute(other, "tp", back_way)
            other = added(other, back_parts[k][side])
        other = lax.ppermute(other, "tp", back_way)
        summed.append(
            (
                total.astype(jnp.float32)
                + other.astype(jnp.float32)
                + part_own[side].astype(jnp.float32)
            ).astype(jnp.bfloat16)
        )
    summed = jnp.concatenate(summed, axis=0)

    returned = lax.all_to_all(summed, "sp", split_axis=0, concat_axis=0, tiled=True)
    combined = stream.astype(jnp.float32)
    for k in range(2):
        picked = jnp.take(returned, own_slots[:, k], axis=0, mode="clip").astype(jnp.float32)
        combined = combined + expert_weights[:, k : k + 1] * picked
    return combined.astype(jnp.bfloat16)


def solution(mesh):
    placed = (
        P("sp", "tp"),
        P("sp", "tp"),
        P("sp", "tp"),
        P("sp", "tp"),
        P("tp", None),
        P("tp", None),
        P(("sp", "tp"), None),
        P(),
        P("sp", None, "tp"),
        P("sp", None, "tp"),
        P("sp", "tp", None),
        P(("sp", "tp"), None),
        P(("sp", "tp"), None),
    )
    return jax.shard_map(
        on_device, mesh=mesh, in_specs=placed, out_specs=P(("sp", "tp"), None), check_vma=False
    )
```
